32 devices in a mesh: kv: 8 (over z, y), tp: 4 (over x, core).
Axes of the slice: x: 2, y: 2, z: 4, core: 2. Of those that a mesh axis runs over, the one named last changes fastest.
Arguments:
- tokens: bfloat16 [48, 24, 4096], P(None, None, 'kv'), may hold values from -6 to 6
- norm_gain: bfloat16 [4096], P('kv'), may hold values from 0.099609375 to 1.8984375
- w_query: bfloat16 [4096, 2048], P('kv', 'tp'), may hold values from -0.09375 to 0.09375
- w_key: bfloat16 [4096, 512], P('kv', 'tp'), may hold values from -0.09375 to 0.09375
- w_value: bfloat16 [4096, 512], P('kv', 'tp'), may hold values from -0.09375 to 0.09375
- w_forget: bfloat16 [4096, 32], replicated, may hold values from -0.09375 to 0.09375
- forget_bias: float32 [32], P('tp'), may hold values from -1 to 3
- query_gain: bfloat16 [64], replicated, may hold values from 0.099609375 to 1.8984375
- key_gain: bfloat16 [64], replicated, may hold values from 0.099609375 to 1.8984375
- w_out: bfloat16 [2048, 4096], P('tp', 'kv'), may hold values from -0.5 to 0.5
- key_cache: bfloat16 [48, 512, 8192], P(None, 'tp', 'kv'), may hold values from -46 to 46
- value_cache: bfloat16 [48, 512, 8192], P(None, 'tp', 'kv'), may hold values from -6 to 6
- gate_sums: float32 [48, 32, 8192], P(None, 'tp', 'kv'), may hold values from -1027 to 0, as said below
- parents: int32 [48, 24], replicated, may hold values from -1 to 22, as said below
- lengths: int32 [48], replicated, may hold values from 4096 to 8186
- accepted: int32 [48], replicated, may hold values from 0 to 6
Outputs:
- mixed: bfloat16 [48, 24, 4096], P(None, None, 'kv')
The draws below stay inside these ranges and needn't reach their ends.
Inputs may be any that keep to these rules, and one draw needn't show every extreme that they name: `gate_sums`: for each sequence and head it never rises along the positions. `parents`: the parent of proposal i is -1 (the cache's last visible position) or one of the proposals i - 3 to i - 1. The accepted proposals stand in the cache right after the first lengths positions.
All inputs are finite; a program needn't handle non-finite values.
Results may differ from the reference program's by a relative error of at most 0.03.
Values may be sent and summed in bfloat16 or wider, within the bound.
A program may use at most 128 MiB of HBM per device.

```python
import jax
import jax.numpy as jnp
from jax import lax

D = 4096
HEADS = 32
KV_HEADS = 8
HEAD_DIM = 64
DRAFT = 24
POS_DEV = 1024
BATCH = 48
LENGTH = 8192
N_TP = 4


def draw_key_cache(key, part):
    base_key, sign_key = jax.random.split(jax.random.fold_in(key, 37), 2)
    noise = jnp.clip(jax.random.normal(base_key, (BATCH, KV_HEADS * HEAD_DIM, LENGTH), jnp.float32), -6.0, 6.0)
    signs = jnp.where(jax.random.bernoulli(sign_key, 0.5, (KV_HEADS * HEAD_DIM,)), 1.0, -1.0)
    first_row = (jnp.arange(BATCH, dtype=jnp.int32) == 0).astype(jnp.float32)
    shift = 40.0 * first_row[:, None, None] * signs[None, :, None]
    return (noise + shift).astype(jnp.bfloat16)


def draw_lengths(key, part):
    low = LENGTH // 2
    span = LENGTH - DRAFT // 4 - low + 1
    picks = jax.random.randint(jax.random.fold_in(key, 41), (BATCH,), 0, span)
    row_ids = jnp.arange(BATCH, dtype=jnp.int32)
    spread = jnp.where(row_ids == 1, picks[0] + span // 2, picks)
    return (low + spread % span).astype(jnp.int32)


def draw_gate_sums(key, part):
    pick_key, fast_key, slow_key, block_key, rough_key, spot_key, loss_key = jax.random.split(jax.random.fold_in(key, 11), 7)
    order = jax.random.permutation(pick_key, HEADS)
    fast_heads = order < HEADS // 2
    fast_rate = jnp.exp(jax.random.uniform(fast_key, (BATCH, HEADS), jnp.float32, jnp.log(1.0 / 50.0), jnp.log(1.0 / 30.0)))
    slow_rate = jax.random.uniform(slow_key, (BATCH, HEADS), jnp.float32, 0.5, 2.0) / LENGTH
    base_rate = jnp.where(fast_heads[None, :], fast_rate, slow_rate)
    block_factor = jnp.exp(jax.random.uniform(block_key, (BATCH, HEADS, LENGTH // POS_DEV), jnp.float32, jnp.log(0.4), jnp.log(2.5)))
    block_factor = jnp.repeat(block_factor, POS_DEV, axis=2)
    rough = jax.random.uniform(rough_key, (BATCH, HEADS, LENGTH), jnp.float32, 0.5, 1.5)
    gate_logarithm = -base_rate[:, :, None] * block_factor * rough
    cache_positions = jax.random.randint(spot_key, (BATCH, 3), 0, LENGTH)
    loss_values = jax.random.uniform(loss_key, (BATCH, HEADS, 3), jnp.float32, 0.2, 0.5)
    slot_positions = jnp.arange(LENGTH, dtype=jnp.int32)
    for draft_group_index in range(3):
        match_flag = slot_positions[None, None, :] == cache_positions[:, None, draft_group_index:draft_group_index + 1]
        gate_logarithm = gate_logarithm + jnp.where(match_flag, jnp.log(1.0 - loss_values[:, :, draft_group_index:draft_group_index + 1]), 0.0)
    return jnp.cumsum(gate_logarithm, axis=2)


def draw_parents(key, part):
    node_ids = jnp.arange(DRAFT, dtype=jnp.int32)
    step_back = jax.random.randint(jax.random.fold_in(key, 23), (BATCH, DRAFT), 1, 4)
    return jnp.maximum(node_ids[None, :] - step_back, -1).astype(jnp.int32)


def plant(entries, own_key, smallest, top_value):
    shape = entries.shape
    spot = [jax.random.randint(jax.random.fold_in(own_key, axis), (), 0, shape[axis]) for axis in range(len(shape))]
    entries = entries.at[tuple(spot)].set(smallest)
    longest = shape.index(max(shape))
    spot[longest] = (spot[longest] + 1) % shape[longest]
    return entries.at[tuple(spot)].set(top_value)


def block_levels(key, shape, cuts, smallest, high):
    factor_of, own = 1.0, jax.random.fold_in(key, 6)
    for axis_at, shards_of in cuts:
        heights = jnp.exp(jax.random.uniform(jax.random.fold_in(own, axis_at), (shards_of,), jnp.float32, smallest / len(cuts), high / len(cuts)))
        factor_of = factor_of * jnp.repeat(heights, shape[axis_at] // shards_of).reshape([-1 if axis == axis_at else 1 for axis in range(len(shape))])
    return factor_of


def scatter_about(stream_key, extent, width, bound, cuts=(), kind=jnp.bfloat16):
    values = jax.random.normal(stream_key, extent, jnp.float32) * width
    if len(cuts) > 0:
        values = block_levels(stream_key, extent, cuts, -0.22, 0.18) * values
    return jnp.clip(values, min=-bound, max=bound).astype(kind)


def setup_inputs(seed: int = 0) -> dict:
    key_list = jax.random.split(jax.random.key(seed), 17)
    tokens = scatter_about(key_list[0], (BATCH, DRAFT, D), 1.0, 6.0, ((2, 8),))
    norm_gain = jnp.clip(1.0 + 0.18 * jax.random.normal(key_list[1], (D,), jnp.float32), 0.099609375, 1.8984375).astype(jnp.bfloat16)
    w_query = scatter_about(key_list[2], (D, HEADS * HEAD_DIM), D ** -0.5, 0.09375, ((0, 8), (1, 4)))
    w_key = scatter_about(key_list[3], (D, KV_HEADS * HEAD_DIM), D ** -0.5, 0.09375, ((0, 8), (1, 4)))
    w_value = scatter_about(key_list[4], (D, KV_HEADS * HEAD_DIM), D ** -0.5, 0.09375, ((0, 8), (1, 4)))
    w_forget = scatter_about(key_list[5], (D, HEADS), D ** -0.5, 0.09375)
    forget_bias = jnp.clip(-1.0 + 4.0 * jax.random.uniform(key_list[6], (HEADS,), jnp.float32) ** block_levels(key_list[6], (HEADS,), ((0, 4),), -0.2, 0.2), -1.0, 3.0)
    query_gain = jnp.clip(1.0 + 0.18 * jax.random.normal(key_list[7], (HEAD_DIM,), jnp.float32), 0.099609375, 1.8984375).astype(jnp.bfloat16)
    key_gain = jnp.clip(1.0 + 0.18 * jax.random.normal(key_list[8], (HEAD_DIM,), jnp.float32), 0.099609375, 1.8984375).astype(jnp.bfloat16)
    w_out = scatter_about(key_list[9], (HEADS * HEAD_DIM, D), (2 * HEAD_DIM) ** -0.5, 0.5, ((0, 4), (1, 8)))
    key_cache = draw_key_cache(jax.random.fold_in(key_list[16], 71), 0)
    value_cache = scatter_about(key_list[11], (BATCH, KV_HEADS * HEAD_DIM, LENGTH), 1.0, 6.0, ((1, 4), (2, 8)))
    gate_sums = draw_gate_sums(jax.random.fold_in(key_list[16], 71), 0)
    parents = draw_parents(jax.random.fold_in(key_list[16], 71), 0)
    lengths = draw_lengths(jax.random.fold_in(key_list[16], 71), 0)
    accepted = plant(jax.random.randint(key_list[15], (BATCH,), 0, DRAFT // 4 + 1), jax.random.fold_in(key_list[15], 1), 0, (DRAFT // 4 + 1) - 1).astype(jnp.int32)
    return dict(tokens=tokens, norm_gain=norm_gain, w_query=w_query, w_key=w_key, w_value=w_value, w_forget=w_forget, forget_bias=forget_bias, query_gain=query_gain, key_gain=key_gain, w_out=w_out, key_cache=key_cache, value_cache=value_cache, gate_sums=gate_sums, parents=parents, lengths=lengths, accepted=accepted)


eps = 1e-05

def head_norm(block, gain):
    mean_sq = lax.optimization_barrier(jnp.mean(block * block, axis=-1, keepdims=True))
    return (block * lax.rsqrt(mean_sq + eps) * gain.astype(jnp.float32)).astype(jnp.bfloat16)

def ancestors(parents, node_count):
    node_ids = jnp.arange(node_count, dtype=jnp.int32)
    reach_map = (parents[:, :, None] == node_ids[None, None, :]).astype(jnp.float32)
    reach_map = reach_map + jnp.eye(node_count, dtype=jnp.float32)[None]
    for repeat_index in range(max(node_count - 1, 1).bit_length()):
        reach_map = jnp.minimum(jnp.einsum('bij,bjk->bik', reach_map, reach_map, precision=lax.Precision.HIGHEST), 1.0)
    return reach_map

def reference(tokens, norm_gain, w_query, w_key, w_value, w_forget, forget_bias, query_gain, key_gain, w_out, key_cache, value_cache, gate_sums, parents, lengths, accepted):
    row_count = BATCH * DRAFT
    group_size = HEADS // KV_HEADS
    scale = HEAD_DIM ** (-0.5)
    wide_rows = tokens.reshape(row_count, D).astype(jnp.float32)
    squares = lax.optimization_barrier(jnp.sum(wide_rows * wide_rows, axis=1))
    inverse = lax.rsqrt(squares / D + eps)
    scaled = (wide_rows * norm_gain.astype(jnp.float32)[None, :]).astype(jnp.bfloat16)

    def project(weight):
        return jnp.dot(scaled, weight, preferred_element_type=jnp.float32) * inverse[:, None]
    query_rows = lax.optimization_barrier(head_norm(project(w_query).reshape(BATCH, DRAFT, HEADS, HEAD_DIM), query_gain))
    keys_new = lax.optimization_barrier(head_norm(project(w_key).reshape(BATCH, DRAFT, KV_HEADS, HEAD_DIM), key_gain))
    values_new = lax.optimization_barrier(project(w_value).astype(jnp.bfloat16)).reshape(BATCH, DRAFT, KV_HEADS, HEAD_DIM)
    gate_logarithm = jax.nn.log_sigmoid(project(w_forget) + forget_bias.astype(jnp.float32)[None, :]).reshape(BATCH, DRAFT, HEADS)
    reach_map = ancestors(parents, DRAFT)
    path_sums = jnp.einsum('bij,bjh->bhi', reach_map, gate_logarithm, precision=lax.Precision.HIGHEST)
    valid_len = lengths + accepted
    slot_positions = jnp.arange(LENGTH, dtype=jnp.int32)

    def one_sequence(items):
        query_seq, key_new, value_new, key_seq, value_seq, gate_seq, path_seq, reach_seq, length_now = items
        query_wide = query_seq.astype(jnp.float32).reshape(DRAFT, KV_HEADS, group_size, HEAD_DIM)
        key_wide = key_seq.astype(jnp.float32).reshape(KV_HEADS, HEAD_DIM, LENGTH)
        gate_last = lax.optimization_barrier(jnp.sum(jnp.where(slot_positions[None, :] == length_now - 1, gate_seq, 0.0), axis=1))
        cache_logits = jnp.einsum('pkgd,kds->kgps', query_wide, key_wide).reshape(HEADS, DRAFT, LENGTH)
        cache_logits = cache_logits * scale + (gate_last[:, None] + path_seq)[:, :, None] - gate_seq[:, None, :]
        cache_logits = jnp.where((slot_positions < length_now)[None, None, :], cache_logits, -jnp.inf)
        new_logits = jnp.einsum('pkgd,jkd->kgpj', query_wide, key_new.astype(jnp.float32)).reshape(HEADS, DRAFT, DRAFT)
        new_logits = new_logits * scale + path_seq[:, :, None] - path_seq[:, None, :]
        new_logits = jnp.where((reach_seq > 0.5)[None], new_logits, -jnp.inf)
        weights = jax.nn.softmax(jnp.concatenate([cache_logits, new_logits], axis=2), axis=2).astype(jnp.bfloat16)
        weights = lax.optimization_barrier(weights).astype(jnp.float32)
        value_rows = jnp.transpose(value_seq.reshape(KV_HEADS, HEAD_DIM, LENGTH), (2, 0, 1))
        value_all = jnp.concatenate([value_rows, value_new], axis=0).astype(jnp.float32)
        attended = jnp.einsum('kgps,skd->pkgd', weights.reshape(KV_HEADS, group_size, DRAFT, LENGTH + DRAFT), value_all)
        return attended.reshape(DRAFT, HEADS * HEAD_DIM).astype(jnp.bfloat16)
    attended = lax.map(one_sequence, (query_rows, keys_new, values_new, key_cache, value_cache, gate_sums, path_sums, reach_map, valid_len))
    attended = lax.optimization_barrier(attended).reshape(row_count, HEADS * HEAD_DIM)
    group_width = HEADS * HEAD_DIM // N_TP
    summed = jnp.zeros((row_count, D), jnp.float32)
    for group_index in range(N_TP):
        group_part = jnp.dot(attended[:, group_index * group_width:(group_index + 1) * group_width], w_out[group_index * group_width:(group_index + 1) * group_width], preferred_element_type=jnp.float32)
        summed = summed + lax.optimization_barrier(group_part.astype(jnp.bfloat16)).astype(jnp.float32)
    return summed.astype(jnp.bfloat16).reshape(BATCH, DRAFT, D)
```

```python
import functools

import jax
import jax.numpy as jnp
from jax import lax
from jax.experimental import pallas as pl
from jax.experimental.pallas import tpu as pltpu
from jax.sharding import PartitionSpec as P

eps = 1e-05
floor_value = -1e30
MESH = pl.DeviceIdType.MESH
NT = (((1,), (1,)), ((), ()))
HIGHEST = lax.Precision.HIGHEST


def greet(axis, size, me):
    barrier = pltpu.get_barrier_semaphore()
    for step in range(1, size):
        pl.semaphore_signal(
            barrier, inc=1, device_id={axis: lax.rem(me + step, size)}, device_id_type=MESH
        )
    pl.semaphore_wait(barrier, size - 1)


def move_kernel(axis, size, count, spread, *refs):
    sources, targets = refs[:count], refs[count : 2 * count]
    send_sem, recv_sem, own_sem = refs[2 * count :]
    me = lax.axis_index(axis)

    def piece(source, index):
        return source.at[index] if spread else source

    own = [
        pltpu.make_async_copy(piece(source, me), target.at[me], own_sem.at[k])
        for k, (source, target) in enumerate(zip(sources, targets))
    ]
    for copy in own:
        copy.start()
    greet(axis, size, me)
    copies = []
    for step in range(1, size):
        peer = lax.rem(me + step, size)
        for k, (source, target) in enumerate(zip(sources, targets)):
            copy = pltpu.make_async_remote_copy(
                src_ref=piece(source, peer),
                dst_ref=target.at[me],
                send_sem=send_sem.at[k, step - 1],
                recv_sem=recv_sem.at[k, step - 1],
                device_id={axis: peer},
                device_id_type=MESH,
            )
            copy.start()
            copies.append(copy)
    for copy in own:
        copy.wait()
    for copy in copies:
        copy.wait()


def move(axis, arrays, spread, ident):
    size = lax.axis_size(axis)
    count = len(arrays)
    shapes = [
        jax.ShapeDtypeStruct(a.shape if spread else (size, *a.shape), a.dtype) for a in arrays
    ]
    return pl.pallas_call(
        functools.partial(move_kernel, axis, size, count, spread),
        out_shape=shapes,
        in_specs=[pl.BlockSpec(memory_space=pl.ANY)] * count,
        out_specs=[pl.BlockSpec(memory_space=pl.ANY)] * count,
        scratch_shapes=[
            pltpu.SemaphoreType.DMA((count, size - 1)),
            pltpu.SemaphoreType.DMA((count, size - 1)),
            pltpu.SemaphoreType.DMA((count,)),
        ],
        compiler_params=pltpu.CompilerParams(collective_id=ident, has_side_effects=True),
        name=f"move{ident}",
    )(*arrays)


def lanes(rows):
    return lax.broadcasted_iota(jnp.int32, (rows, 128), 1)


def paired_norm(block, gain, low):
    squares = block * block
    first = jnp.sum(jnp.where(low, squares, 0.0), axis=1, keepdims=True)
    second = jnp.sum(jnp.where(low, 0.0, squares), axis=1, keepdims=True)
    mean_sq = jnp.where(low, first, second) * (1.0 / 64)
    return block * lax.rsqrt(mean_sq + eps) * gain


def finish_kernel(size, model_width, rounds, groups, sides, parts, parent, params, q_out, o_out, s_out):
    rows = q_out.shape[0]
    width = groups * 128
    lane = lanes(rows)
    low = lane < 64

    def total_of(start):
        piece = parts[0, :, start : start + 128].astype(jnp.float32)
        for j in range(1, size):
            piece = piece + parts[j, :, start : start + 128].astype(jnp.float32)
        return piece

    gate = total_of(width + 256)
    heads = sides * groups
    squares = jnp.sum(
        jnp.where((lane == heads) | (lane == heads + 1), gate, 0.0), axis=1, keepdims=True
    )
    inverse = lax.rsqrt(squares * (1.0 / model_width) + eps)
    query = []
    for g in range(groups):
        normed = paired_norm(total_of(128 * g) * inverse, params[0:1, :], low).astype(jnp.bfloat16)
        q_out[:, 128 * g : 128 * g + 128] = normed
        query.append(normed.astype(jnp.float32))
    keys = paired_norm(total_of(width) * inverse, params[1:2, :], low).astype(jnp.bfloat16)
    values = (total_of(width + 128) * inverse).astype(jnp.bfloat16)
    pre = jnp.where(lane < heads, gate * inverse + params[2:3, :], 0.0)
    log_gate = jnp.minimum(pre, 0.0) - jnp.log1p(jnp.exp(-jnp.abs(pre)))
    row_id = lax.broadcasted_iota(jnp.int32, (rows, rows), 0)
    col_id = lax.broadcasted_iota(jnp.int32, (rows, rows), 1)
    reach = jnp.where((col_id == row_id) | (col_id == parent[...]), 1.0, 0.0)
    for _ in range(rounds):
        half = reach.astype(jnp.bfloat16)
        reach = jnp.minimum(jnp.dot(half, half, preferred_element_type=jnp.float32), 1.0)
    path = jnp.dot(reach, log_gate, precision=HIGHEST, preferred_element_type=jnp.float32)
    pick = jnp.where(lanes(8) == lax.broadcasted_iota(jnp.int32, (8, 128), 0), 1.0, 0.0)
    path_t = lax.dot_general(pick, path, NT, precision=HIGHEST, preferred_element_type=jnp.float32)
    stats = jnp.zeros((rows, 128), jnp.float32)
    for g in range(groups):
        outs = []
        for side in range(sides):
            h = side * groups + g
            mine = low if side == 0 else lane >= 64
            q = jnp.where(mine, query[g] * 0.125, 0.0).astype(jnp.bfloat16)
            logits = lax.dot_general(q, keys, NT, preferred_element_type=jnp.float32)
            logits = jnp.where(reach > 0.5, logits - path_t[h : h + 1, :], floor_value)
            top = jnp.max(logits, axis=1, keepdims=True)
            weights = jnp.exp(logits - top)
            total = jnp.sum(weights, axis=1, keepdims=True)
            out = jnp.dot(weights.astype(jnp.bfloat16), values, preferred_element_type=jnp.float32)
            outs.append(out / total)
            stats = jnp.where(lane == h, top, jnp.where(lane == heads + h, total, stats))
        o_out[:, 128 * g : 128 * g + 128] = jnp.where(low, outs[0], outs[-1])
    s_out[...] = stats


def attend_kernel(batch, groups, sides, drafts, valid_ref, q_ref, k_ref, v_ref, g_ref, o_ref, s_ref):
    positions = k_ref.shape[2]
    heads = sides * groups
    base = lax.axis_index("kv") * positions
    lane = lanes(drafts)
    low = lane < 64
    place = lax.broadcasted_iota(jnp.int32, (heads, positions), 1)
    for b in range(batch):
        valid = valid_ref[pl.program_id(0) * batch + b] - base
        gates = g_ref[b]
        last = jnp.sum(jnp.where(place == valid - 1, gates, 0.0), axis=1, keepdims=True)
        gates = jnp.where(place < valid, gates, -floor_value)
        query = q_ref[b].astype(jnp.float32) * 0.125
        pieces = [query[:, 128 * g : 128 * g + 128] for g in range(groups)]
        if sides == 2:
            pieces = [jnp.where(low, p, 0.0) for p in pieces] + [
                jnp.where(low, 0.0, p) for p in pieces
            ]
        else:
            pieces = [p[:, :64] for p in pieces]
        wide = jnp.concatenate(pieces, axis=0).astype(jnp.bfloat16)
        logits = jnp.dot(wide, k_ref[b], preferred_element_type=jnp.float32)
        logits = logits.reshape(heads, drafts, positions) - gates[:, None, :]
        top = jnp.max(logits, axis=2, keepdims=True)
        weights = jnp.exp(logits - top)
        total = jnp.sum(weights, axis=2, keepdims=True)
        flat = weights.reshape(heads * drafts, positions).astype(jnp.bfloat16)
        out = lax.dot_general(flat, v_ref[b], NT, preferred_element_type=jnp.float32)
        if sides == 1:
            out = jnp.concatenate([out, jnp.zeros_like(out)], axis=1)
        out = out.reshape(heads, drafts, 128) / total
        stats = jnp.zeros((drafts, 128), jnp.float32)
        for h in range(heads):
            stats = jnp.where(lane == h, top[h], stats)
            stats = jnp.where(lane == heads + h, total[h], stats)
            stats = jnp.where(lane == 2 * heads + h, last[h : h + 1, :], stats)
        s_ref[b] = stats
        for g in range(groups):
            o_ref[b, :, 128 * g : 128 * g + 128] = jnp.where(
                low, out[g], out[(sides - 1) * groups + g]
            ).astype(jnp.bfloat16)


def merge_kernel(size, groups, sides, sums, stats, o_new, s_new, out):
    rows = out.shape[0]
    heads = sides * groups
    low = lanes(rows) < 64
    both = stats[0]
    for j in range(1, size):
        both = both + stats[j]
    last = pltpu.roll(both, 128 - 2 * heads, 1)
    tops = [stats[j] for j in range(size)] + [s_new[...] - last]
    totals = [pltpu.roll(stats[j], 128 - heads, 1) for j in range(size)]
    totals.append(pltpu.roll(s_new[...], 128 - heads, 1))
    top = functools.reduce(jnp.maximum, tops)
    shares = [jnp.exp(t - top) * n for t, n in zip(tops, totals)]
    norm = 1.0 / functools.reduce(jnp.add, shares)
    shares = [s * norm for s in shares]
    for g in range(groups):
        span = slice(128 * g, 128 * g + 128)
        acc = jnp.zeros((rows, 128), jnp.float32)
        for j, share in enumerate(shares):
            block = o_new[:, span] if j == size else sums[j, :, span].astype(jnp.float32)
            other = (sides - 1) * groups + g
            factor = jnp.where(low, share[:, g : g + 1], share[:, other : other + 1])
            acc = acc + factor * block
        out[:, span] = acc.astype(jnp.bfloat16)


def body(
    tokens,
    norm_gain,
    w_query,
    w_key,
    w_value,
    w_forget,
    forget_bias,
    query_gain,
    key_gain,
    w_out,
    key_cache,
    value_cache,
    gate_sums,
    parents,
    lengths,
    accepted,
):
    seq_count, drafts, local_width = tokens.shape
    row_count = seq_count * drafts
    head_dim = query_gain.shape[0]
    heads = forget_bias.shape[0]
    sides = w_key.shape[1] // head_dim
    groups = heads // sides
    positions = key_cache.shape[2]
    size, tp_size = lax.axis_size("kv"), lax.axis_size("tp")
    kv_index, tp_index = lax.axis_index("kv"), lax.axis_index("tp")
    model_width = local_width * size
    share = row_count // size
    query_width = 2 * groups * head_dim
    f32, bf16 = jnp.float32, jnp.bfloat16

    wide_rows = tokens.reshape(row_count, local_width).astype(f32)
    squares = jnp.sum(wide_rows * wide_rows, axis=1, keepdims=True)
    coarse = squares.astype(bf16).astype(f32)
    scaled = (wide_rows * norm_gain.astype(f32)[None, :]).astype(bf16)
    forget_rows = lax.dynamic_slice(
        w_forget, (kv_index * local_width, tp_index * heads), (local_width, heads)
    )
    w_pairs = w_query.reshape(local_width, sides, groups, head_dim).transpose(0, 2, 1, 3)
    w_pairs = jnp.pad(w_pairs, ((0, 0), (0, 0), (0, 2 - sides), (0, 0)))
    w_pairs = w_pairs.reshape(local_width, query_width)
    fill = ((0, 0), (0, 128 - sides * head_dim))
    w_all = jnp.concatenate(
        [w_pairs, jnp.pad(w_key, fill), jnp.pad(w_value, fill), jnp.pad(forget_rows, ((0, 0), (0, 128 - heads)))], axis=1
    )
    partial = jnp.dot(scaled, w_all, preferred_element_type=f32)
    column = jnp.arange(partial.shape[1])[None, :] - (query_width + 256)
    partial = jnp.where(
        column == heads, coarse, jnp.where(column == heads + 1, squares - coarse, partial)
    ).astype(bf16)
    (parts,) = move("kv", [partial.reshape(size, share, -1)], True, 0)

    params = jnp.stack(
        [
            jnp.tile(query_gain.astype(f32), 2),
            jnp.tile(key_gain.astype(f32), 2),
            jnp.pad(forget_bias, (0, 128 - heads)),
        ]
    )
    params = jnp.pad(params, ((0, 5), (0, 0)))
    seq_share = seq_count // size
    own_parents = lax.dynamic_slice(parents, (kv_index * seq_share, 0), (seq_share, drafts))
    starts = jnp.arange(seq_share, dtype=jnp.int32)[:, None] * drafts
    parent_rows = jnp.where(own_parents < 0, -1, own_parents + starts).reshape(share, 1)
    rounds = max(drafts - 1, 1).bit_length()
    query, o_new, s_new = pl.pallas_call(
        functools.partial(finish_kernel, size, model_width, rounds, groups, sides),
        out_shape=[
            jax.ShapeDtypeStruct((share, query_width), bf16),
            jax.ShapeDtypeStruct((share, query_width), f32),
            jax.ShapeDtypeStruct((share, 128), f32),
        ],
        name="finish",
    )(parts, parent_rows, params)
    (query_all,) = move("kv", [query], False, 1)

    batch = 4 if seq_count % 4 == 0 else 1
    valid = lengths + accepted
    by_seq = lambda i, *_: (i, 0, 0)
    weighted, stats = pl.pallas_call(
        functools.partial(attend_kernel, batch, groups, sides, drafts),
        out_shape=[
            jax.ShapeDtypeStruct((seq_count, drafts, query_width), bf16),
            jax.ShapeDtypeStruct((seq_count, drafts, 128), f32),
        ],
        grid_spec=pltpu.PrefetchScalarGridSpec(
            num_scalar_prefetch=1,
            grid=(seq_count // batch,),
            in_specs=[
                pl.BlockSpec((batch, drafts, query_width), by_seq),
                pl.BlockSpec((batch, key_cache.shape[1], positions), by_seq),
                pl.BlockSpec((batch, key_cache.shape[1], positions), by_seq),
                pl.BlockSpec((batch, heads, positions), by_seq),
            ],
            out_specs=[
                pl.BlockSpec((batch, drafts, query_width), by_seq),
                pl.BlockSpec((batch, drafts, 128), by_seq),
            ],
        ),
        name="attend",
    )(
        valid,
        query_all.reshape(seq_count, drafts, query_width),
        key_cache,
        value_cache,
        gate_sums,
    )
    sums, stats_all = move(
        "kv", [weighted.reshape(size, share, query_width), stats.reshape(size, share, 128)], True, 2
    )
    attended = pl.pallas_call(
        functools.partial(merge_kernel, size, groups, sides),
        out_shape=jax.ShapeDtypeStruct((share, query_width), bf16),
        name="merge",
    )(sums, stats_all, o_new, s_new)
    (attended,) = move("kv", [attended], False, 3)
    w_rows = w_out.reshape(sides, groups, head_dim, -1).transpose(1, 0, 2, 3)
    w_rows = jnp.pad(w_rows, ((0, 0), (0, 2 - sides), (0, 0), (0, 0))).reshape(query_width, -1)
    partial_out = jnp.dot(
        attended.reshape(row_count, query_width), w_rows, preferred_element_type=f32
    ).astype(bf16)
    (pieces,) = move("tp", [partial_out.reshape(tp_size, row_count // tp_size, -1)], True, 4)
    mixed = jnp.sum(pieces.astype(f32), axis=0).astype(bf16)
    (mixed,) = move("tp", [mixed], False, 5)
    return mixed.reshape(seq_count, drafts, local_width)


def solution(mesh):
    return jax.shard_map(
        body,
        mesh=mesh,
        in_specs=(
            P(None, None, "kv"),
            P("kv"),
            P("kv", "tp"),
            P("kv", "tp"),
            P("kv", "tp"),
            P(),
            P("tp"),
            P(),
            P(),
            P("tp", "kv"),
            P(None, "tp", "kv"),
            P(None, "tp", "kv"),
            P(None, "tp", "kv"),
            P(),
            P(),
            P(),
        ),
        out_specs=P(None, None, "kv"),
        check_vma=False,
    )
```

```python
import functools

import jax
import jax.numpy as jnp
from jax import lax
from jax.experimental import pallas as pl
from jax.experimental.pallas import tpu as pltpu
from jax.sharding import PartitionSpec as P

eps = 1e-05
floor_value = -1e30
MESH = pl.DeviceIdType.MESH
NT = (((1,), (1,)), ((), ()))
HIGHEST = lax.Precision.HIGHEST


def greet(axis, size, me):
    barrier = pltpu.get_barrier_semaphore()
    for step in range(1, size):
        pl.semaphore_signal(
            barrier, inc=1, device_id={axis: lax.rem(me + step, size)}, device_id_type=MESH
        )
    pl.semaphore_wait(barrier, size - 1)


def move_kernel(axis, size, count, *refs):
    sources, targets = refs[:count], refs[count : 2 * count]
    send_sem, recv_sem, own_sem = refs[2 * count :]
    me = lax.axis_index(axis)

    own = [
        pltpu.make_async_copy(source.at[me], target.at[me], own_sem.at[k])
        for k, (source, target) in enumerate(zip(sources, targets))
    ]
    for copy in own:
        copy.start()
    greet(axis, size, me)
    copies = []
    for step in range(1, size):
        peer = lax.rem(me + step, size)
        for k, (source, target) in enumerate(zip(sources, targets)):
            copy = pltpu.make_async_remote_copy(
                src_ref=source.at[peer],
                dst_ref=target.at[me],
                send_sem=send_sem.at[k, step - 1],
                recv_sem=recv_sem.at[k, step - 1],
                device_id={axis: peer},
                device_id_type=MESH,
            )
            copy.start()
            copies.append(copy)
    for copy in own:
        copy.wait()
    for copy in copies:
        copy.wait()


def move(axis, arrays, ident):
    size = lax.axis_size(axis)
    count = len(arrays)
    shapes = [jax.ShapeDtypeStruct(a.shape, a.dtype) for a in arrays]
    return pl.pallas_call(
        functools.partial(move_kernel, axis, size, count),
        out_shape=shapes,
        in_specs=[pl.BlockSpec(memory_space=pl.ANY)] * count,
        out_specs=[pl.BlockSpec(memory_space=pl.ANY)] * count,
        scratch_shapes=[
            pltpu.SemaphoreType.DMA((count, size - 1)),
            pltpu.SemaphoreType.DMA((count, size - 1)),
            pltpu.SemaphoreType.DMA((count,)),
        ],
        compiler_params=pltpu.CompilerParams(collective_id=ident, has_side_effects=True),
        name=f"move{ident}",
    )(*arrays)


def gather_kernel(axis, size, source, target, pair_send, pair_recv, far_send, far_recv, own_sem):
    me = lax.axis_index(axis)
    partner = me + 1 - 2 * lax.rem(me, 2)
    half = size // 2
    column = [lax.rem(me + 2 * step, size) for step in range(1, half)]
    own = pltpu.make_async_copy(source, target.at[me], own_sem)
    own.start()
    barrier = pltpu.get_barrier_semaphore()
    for peer in [partner] + column:
        pl.semaphore_signal(barrier, inc=1, device_id={axis: peer}, device_id_type=MESH)
    pl.semaphore_wait(barrier, half)

    def send(block, slot, sems, index, peer):
        copy = pltpu.make_async_remote_copy(
            src_ref=block,
            dst_ref=target.at[slot],
            send_sem=sems[0].at[index],
            recv_sem=sems[1].at[index],
            device_id={axis: peer},
            device_id_type=MESH,
        )
        copy.start()
        return copy

    near_sems, far_sems = (pair_send, pair_recv), (far_send, far_recv)
    far = [send(source, me, far_sems, k, peer) for k, peer in enumerate(column)]
    near = [send(source, me, near_sems, 0, partner)]
    for k, copy in enumerate(far):
        copy.wait_recv()
        origin = lax.rem(me + size - 2 * (k + 1), size)
        near.append(send(target.at[origin], origin, near_sems, k + 1, partner))
    own.wait()
    for copy in far:
        copy.wait_send()
    for copy in near:
        copy.wait()


def gather(axis, array, ident):
    size = lax.axis_size(axis)
    half = size // 2
    return pl.pallas_call(
        functools.partial(gather_kernel, axis, size),
        out_shape=jax.ShapeDtypeStruct((size, *array.shape), array.dtype),
        in_specs=[pl.BlockSpec(memory_space=pl.ANY)],
        out_specs=pl.BlockSpec(memory_space=pl.ANY),
        scratch_shapes=[
            pltpu.SemaphoreType.DMA((half,)),
            pltpu.SemaphoreType.DMA((half,)),
            pltpu.SemaphoreType.DMA((half - 1,)),
            pltpu.SemaphoreType.DMA((half - 1,)),
            pltpu.SemaphoreType.DMA,
        ],
        compiler_params=pltpu.CompilerParams(collective_id=ident, has_side_effects=True),
        name=f"gather{ident}",
    )(array)


def lanes(rows):
    return lax.broadcasted_iota(jnp.int32, (rows, 128), 1)


def paired_norm(block, gain, low):
    squares = block * block
    first = jnp.sum(jnp.where(low, squares, 0.0), axis=1, keepdims=True)
    second = jnp.sum(jnp.where(low, 0.0, squares), axis=1, keepdims=True)
    mean_sq = jnp.where(low, first, second) * (1.0 / 64)
    return block * lax.rsqrt(mean_sq + eps) * gain


def finish_kernel(size, model_width, rounds, groups, sides, parts, parent, params, q_out, o_out, s_out):
    rows = q_out.shape[0]
    width = groups * 128
    lane = lanes(rows)
    low = lane < 64

    def total_of(start):
        piece = parts[0, :, start : start + 128].astype(jnp.float32)
        for j in range(1, size):
            piece = piece + parts[j, :, start : start + 128].astype(jnp.float32)
        return piece

    gate = total_of(width + 256)
    heads = sides * groups
    squares = jnp.sum(
        jnp.where((lane == heads) | (lane == heads + 1), gate, 0.0), axis=1, keepdims=True
    )
    inverse = lax.rsqrt(squares * (1.0 / model_width) + eps)
    query = []
    for g in range(groups):
        normed = paired_norm(total_of(128 * g) * inverse, params[0:1, :], low).astype(jnp.bfloat16)
        q_out[:, 128 * g : 128 * g + 128] = normed
        query.append(normed.astype(jnp.float32))
    keys = paired_norm(total_of(width) * inverse, params[1:2, :], low).astype(jnp.bfloat16)
    values = (total_of(width + 128) * inverse).astype(jnp.bfloat16)
    pre = jnp.where(lane < heads, gate * inverse + params[2:3, :], 0.0)
    log_gate = jnp.minimum(pre, 0.0) - jnp.log1p(jnp.exp(-jnp.abs(pre)))
    row_id = lax.broadcasted_iota(jnp.int32, (rows, rows), 0)
    col_id = lax.broadcasted_iota(jnp.int32, (rows, rows), 1)
    reach = jnp.where((col_id == row_id) | (col_id == parent[...]), 1.0, 0.0)
    for _ in range(rounds):
        half = reach.astype(jnp.bfloat16)
        reach = jnp.minimum(jnp.dot(half, half, preferred_element_type=jnp.float32), 1.0)
    path = jnp.dot(reach, log_gate, precision=HIGHEST, preferred_element_type=jnp.float32)
    pick = jnp.where(lanes(8) == lax.broadcasted_iota(jnp.int32, (8, 128), 0), 1.0, 0.0)
    path_t = lax.dot_general(pick, path, NT, precision=HIGHEST, preferred_element_type=jnp.float32)
    stats = jnp.zeros((rows, 128), jnp.float32)
    for g in range(groups):
        outs = []
        for side in range(sides):
            h = side * groups + g
            mine = low if side == 0 else lane >= 64
            q = jnp.where(mine, query[g] * 0.125, 0.0).astype(jnp.bfloat16)
            logits = lax.dot_general(q, keys, NT, preferred_element_type=jnp.float32)
            logits = jnp.where(reach > 0.5, logits - path_t[h : h + 1, :], floor_value)
            top = jnp.max(logits, axis=1, keepdims=True)
            weights = jnp.exp(logits - top)
            total = jnp.sum(weights, axis=1, keepdims=True)
            out = jnp.dot(weights.astype(jnp.bfloat16), values, preferred_element_type=jnp.float32)
            outs.append(out / total)
            stats = jnp.where(lane == h, top, jnp.where(lane == heads + h, total, stats))
        o_out[:, 128 * g : 128 * g + 128] = jnp.where(low, outs[0], outs[-1])
    s_out[...] = stats


def attend_kernel(batch, groups, sides, drafts, valid_ref, q_ref, k_ref, v_ref, g_ref, o_ref, s_ref):
    positions = k_ref.shape[2]
    heads = sides * groups
    base = lax.axis_index("kv") * positions
    lane = lanes(drafts)
    low = lane < 64
    place = lax.broadcasted_iota(jnp.int32, (heads, positions), 1)
    for b in range(batch):
        valid = valid_ref[pl.program_id(0) * batch + b] - base
        gates = g_ref[b]
        last = jnp.sum(jnp.where(place == valid - 1, gates, 0.0), axis=1, keepdims=True)
        gates = jnp.where(place < valid, gates, -floor_value)
        query = q_ref[b].astype(jnp.float32) * 0.125
        pieces = [query[:, 128 * g : 128 * g + 128] for g in range(groups)]
        if sides == 2:
            pieces = [jnp.where(low, p, 0.0) for p in pieces] + [
                jnp.where(low, 0.0, p) for p in pieces
            ]
        else:
            pieces = [p[:, :64] for p in pieces]
        wide = jnp.concatenate(pieces, axis=0).astype(jnp.bfloat16)
        logits = jnp.dot(wide, k_ref[b], preferred_element_type=jnp.float32)
        logits = logits.reshape(heads, drafts, positions) - gates[:, None, :]
        top = jnp.max(logits, axis=2, keepdims=True)
        weights = jnp.exp(logits - top)
        total = jnp.sum(weights, axis=2, keepdims=True)
        flat = weights.reshape(heads * drafts, positions).astype(jnp.bfloat16)
        out = lax.dot_general(flat, v_ref[b], NT, preferred_element_type=jnp.float32)
        if sides == 1:
            out = jnp.concatenate([out, jnp.zeros_like(out)], axis=1)
        out = out.reshape(heads, drafts, 128) / total
        stats = jnp.zeros((drafts, 128), jnp.float32)
        for h in range(heads):
            stats = jnp.where(lane == h, top[h], stats)
            stats = jnp.where(lane == heads + h, total[h], stats)
            stats = jnp.where(lane == 2 * heads + h, last[h : h + 1, :], stats)
        s_ref[b] = stats
        for g in range(groups):
            o_ref[b, :, 128 * g : 128 * g + 128] = jnp.where(
                low, out[g], out[(sides - 1) * groups + g]
            ).astype(jnp.bfloat16)


def merge_kernel(size, groups, sides, sums, stats, o_new, s_new, out):
    rows = out.shape[0]
    heads = sides * groups
    low = lanes(rows) < 64
    both = stats[0]
    for j in range(1, size):
        both = both + stats[j]
    last = pltpu.roll(both, 128 - 2 * heads, 1)
    tops = [stats[j] for j in range(size)] + [s_new[...] - last]
    totals = [pltpu.roll(stats[j], 128 - heads, 1) for j in range(size)]
    totals.append(pltpu.roll(s_new[...], 128 - heads, 1))
    top = functools.reduce(jnp.maximum, tops)
    shares = [jnp.exp(t - top) * n for t, n in zip(tops, totals)]
    norm = 1.0 / functools.reduce(jnp.add, shares)
    shares = [s * norm for s in shares]
    for g in range(groups):
        span = slice(128 * g, 128 * g + 128)
        acc = jnp.zeros((rows, 128), jnp.float32)
        for j, share in enumerate(shares):
            block = o_new[:, span] if j == size else sums[j, :, span].astype(jnp.float32)
            other = (sides - 1) * groups + g
            factor = jnp.where(low, share[:, g : g + 1], share[:, other : other + 1])
            acc = acc + factor * block
        out[:, span] = acc.astype(jnp.bfloat16)


def body(
    tokens,
    norm_gain,
    w_query,
    w_key,
    w_value,
    w_forget,
    forget_bias,
    query_gain,
    key_gain,
    w_out,
    key_cache,
    value_cache,
    gate_sums,
    parents,
    lengths,
    accepted,
):
    seq_count, drafts, local_width = tokens.shape
    row_count = seq_count * drafts
    head_dim = query_gain.shape[0]
    heads = forget_bias.shape[0]
    sides = w_key.shape[1] // head_dim
    groups = heads // sides
    positions = key_cache.shape[2]
    size, tp_size = lax.axis_size("kv"), lax.axis_size("tp")
    kv_index, tp_index = lax.axis_index("kv"), lax.axis_index("tp")
    model_width = local_width * size
    share = row_count // size
    query_width = 2 * groups * head_dim
    f32, bf16 = jnp.float32, jnp.bfloat16

    wide_rows = tokens.reshape(row_count, local_width).astype(f32)
    squares = jnp.sum(wide_rows * wide_rows, axis=1, keepdims=True)
    coarse = squares.astype(bf16).astype(f32)
    scaled = (wide_rows * norm_gain.astype(f32)[None, :]).astype(bf16)
    forget_rows = lax.dynamic_slice(
        w_forget, (kv_index * local_width, tp_index * heads), (local_width, heads)
    )
    w_pairs = w_query.reshape(local_width, sides, groups, head_dim).transpose(0, 2, 1, 3)
    w_pairs = jnp.pad(w_pairs, ((0, 0), (0, 0), (0, 2 - sides), (0, 0)))
    w_pairs = w_pairs.reshape(local_width, query_width)
    fill = ((0, 0), (0, 128 - sides * head_dim))
    w_all = jnp.concatenate(
        [w_pairs, jnp.pad(w_key, fill), jnp.pad(w_value, fill), jnp.pad(forget_rows, ((0, 0), (0, 128 - heads)))], axis=1
    )
    partial = jnp.dot(scaled, w_all, preferred_element_type=f32)
    column = jnp.arange(partial.shape[1])[None, :] - (query_width + 256)
    partial = jnp.where(
        column == heads, coarse, jnp.where(column == heads + 1, squares - coarse, partial)
    ).astype(bf16)
    (parts,) = move("kv", [partial.reshape(size, share, -1)], 0)

    params = jnp.stack(
        [
            jnp.tile(query_gain.astype(f32), 2),
            jnp.tile(key_gain.astype(f32), 2),
            jnp.pad(forget_bias, (0, 128 - heads)),
        ]
    )
    params = jnp.pad(params, ((0, 5), (0, 0)))
    seq_share = seq_count // size
    own_parents = lax.dynamic_slice(parents, (kv_index * seq_share, 0), (seq_share, drafts))
    starts = jnp.arange(seq_share, dtype=jnp.int32)[:, None] * drafts
    parent_rows = jnp.where(own_parents < 0, -1, own_parents + starts).reshape(share, 1)
    rounds = max(drafts - 1, 1).bit_length()
    query, o_new, s_new = pl.pallas_call(
        functools.partial(finish_kernel, size, model_width, rounds, groups, sides),
        out_shape=[
            jax.ShapeDtypeStruct((share, query_width), bf16),
            jax.ShapeDtypeStruct((share, query_width), f32),
            jax.ShapeDtypeStruct((share, 128), f32),
        ],
        name="finish",
    )(parts, parent_rows, params)
    query_all = gather("kv", query, 1)

    batch = 4 if seq_count % 4 == 0 else 1
    valid = lengths + accepted
    by_seq = lambda i, *_: (i, 0, 0)
    weighted, stats = pl.pallas_call(
        functools.partial(attend_kernel, batch, groups, sides, drafts),
        out_shape=[
            jax.ShapeDtypeStruct((seq_count, drafts, query_width), bf16),
            jax.ShapeDtypeStruct((seq_count, drafts, 128), f32),
        ],
        grid_spec=pltpu.PrefetchScalarGridSpec(
            num_scalar_prefetch=1,
            grid=(seq_count // batch,),
            in_specs=[
                pl.BlockSpec((batch, drafts, query_width), by_seq),
                pl.BlockSpec((batch, key_cache.shape[1], positions), by_seq),
                pl.BlockSpec((batch, key_cache.shape[1], positions), by_seq),
                pl.BlockSpec((batch, heads, positions), by_seq),
            ],
            out_specs=[
                pl.BlockSpec((batch, drafts, query_width), by_seq),
                pl.BlockSpec((batch, drafts, 128), by_seq),
            ],
        ),
        name="attend",
    )(
        valid,
        query_all.reshape(seq_count, drafts, query_width),
        key_cache,
        value_cache,
        gate_sums,
    )
    sums, stats_all = move(
        "kv", [weighted.reshape(size, share, query_width), stats.reshape(size, share, 128)], 2
    )
    attended = pl.pallas_call(
        functools.partial(merge_kernel, size, groups, sides),
        out_shape=jax.ShapeDtypeStruct((share, query_width), bf16),
        name="merge",
    )(sums, stats_all, o_new, s_new)
    attended = gather("kv", attended, 3)
    w_rows = w_out.reshape(sides, groups, head_dim, -1).transpose(1, 0, 2, 3)
    w_rows = jnp.pad(w_rows, ((0, 0), (0, 2 - sides), (0, 0), (0, 0))).reshape(query_width, -1)
    partial_out = jnp.dot(
        attended.reshape(row_count, query_width), w_rows, preferred_element_type=f32
    ).astype(bf16)
    (pieces,) = move("tp", [partial_out.reshape(tp_size, row_count // tp_size, -1)], 4)
    mixed = jnp.sum(pieces.astype(f32), axis=0).astype(bf16)
    mixed = gather("tp", mixed, 5)
    return mixed.reshape(seq_count, drafts, local_width)


def solution(mesh):
    return jax.shard_map(
        body,
        mesh=mesh,
        in_specs=(
            P(None, None, "kv"),
            P("kv"),
            P("kv", "tp"),
            P("kv", "tp"),
            P("kv", "tp"),
            P(),
            P("tp"),
            P(),
            P(),
            P("tp", "kv"),
            P(None, "tp", "kv"),
            P(None, "tp", "kv"),
            P(None, "tp", "kv"),
            P(),
            P(),
            P(),
        ),
        out_specs=P(None, None, "kv"),
        check_vma=False,
    )
```
